32 devices in a mesh: grp: 2 (over y), fs: 4 (over z), tp: 4 (over x, core).
Axes of the slice: x: 2, y: 2, z: 4, core: 2. Of those that a mesh axis runs over, the one named last changes fastest.
Arguments:
- tokens: bfloat16 [1024, 2048], P(('grp', 'fs'), 'tp'), parts along dimension 0, may hold values from -340 to 340
- routes: int32 [1024, 2], P(('grp', 'fs')), parts along dimension 0, may hold values from 0 to 7, all different within a row; in each aligned block of 128 rows (0 to 127, 128 to 255, ...) at most 40 rows name the same one
- route_weights: float32 [1024, 2], P(('grp', 'fs')), parts along dimension 0, may hold values from 0.2 to 1
- norm_gain: float32 [2048], P('fs'), may hold values from 0.1 to 1.9
- gate_weight: float32 [8, 2048, 4096], P(None, 'fs', 'tp'), may hold values from -0.125 to 0.125
- up_weight: float32 [8, 2048, 4096], P(None, 'fs', 'tp'), may hold values from -0.125 to 0.125
- down_weight: float32 [8, 2048, 4096], P(None, 'fs', 'tp'), may hold values from -0.09375 to 0.09375
Outputs:
- gate_out: bfloat16 [8, 4096, 4096], P('fs', 'grp', 'tp'), parts along dimension 1
- up_out: bfloat16 [8, 4096, 4096], P('fs', 'grp', 'tp'), parts along dimension 1
- down_out: bfloat16 [8, 4096, 4096], P('fs', 'grp', 'tp'), parts along dimension 1
- mixed_out: bfloat16 [1024, 2048], P(('grp', 'fs'), 'tp'), parts along dimension 0
The draws below stay inside these ranges and needn't reach their ends.
There are 2 independent parts, one for each index of `grp`. The reference program is written for one: setup_inputs(seed, part) draws one part's arguments, and reference() takes and returns one part's arrays. A program takes and returns all parts, laid end to end along the dimension named above; an argument that names none is the same for every part. Nothing has to cross between parts.
Inputs may be any that keep to these rules, and one draw needn't show every extreme that they name: `routes`: each row names 2 different experts; in each aligned block of 128 rows no expert is named by more than 40 rows, and in some block one expert is named by exactly 40 rows.
All inputs are finite; a program needn't handle non-finite values.
Results may differ from the reference program's by a relative error of at most 0.015.
Values may be sent and summed in bfloat16 or wider, within the bound.
A program may use at most 192 MiB of HBM per device.

```python
import math
import jax
import jax.numpy as jnp
import numpy as np
from jax import lax

D = 2048
FF = 4096
EXPERTS = 8
TOP = 2
TOK_FS = 128
CAP = 40
SUB = 1
FFS = 1024
TOKENS = 512
N_FS = 4
N_TP = 4


def draw_tokens(key, part):
    noise_key, column_key, row_key = jax.random.split(key, 3)
    columns = jnp.arange(D, dtype=jnp.float32) / D
    column_scale = jnp.exp(math.log(4.0) * columns) * jax.random.uniform(column_key, (D,), jnp.float32, 0.6, 1.4)
    row_scale = jnp.exp(jax.random.uniform(row_key, (TOKENS, 1), jnp.float32, 0.0, math.log(10.0)))
    values = jnp.clip(jax.random.normal(noise_key, (TOKENS, D), jnp.float32), -6.0, 6.0)
    return (values * column_scale[None, :] * row_scale).astype(jnp.bfloat16)


def block_levels(stream_key, extent, cuts, least, top_value):
    loudness, own = 1.0, jax.random.fold_in(stream_key, 6)
    for axis_at, shards_of in cuts:
        steps = jnp.exp(jax.random.uniform(jax.random.fold_in(own, axis_at), (shards_of,), jnp.float32, least / len(cuts), top_value / len(cuts)))
        loudness = loudness * jnp.repeat(steps, extent[axis_at] // shards_of).reshape([-1 if axis == axis_at else 1 for axis in range(len(extent))])
    return loudness


def assign_block(own_key, own, number, rows, count, top, limit, skew):
    order = jax.random.permutation(own_key, count)
    crowded, ordinary = shares(count, rows * top, limit, skew, True), shares(count, rows * top, limit, skew, False)
    places = jnp.arange(count)

    def named(sizes, rotation):
        used = int((sizes > 0).sum())
        fixed = max(1, used // 4)
        shifted = fixed + (places - fixed + rotation * (used - fixed)) % max(1, count - fixed)
        return jnp.zeros((count,), jnp.int32).at[order[jnp.where(places < fixed, places, shifted)]].set(jnp.asarray(sizes, jnp.int32))

    sizes = jnp.where(number % 4 == 0, named(crowded, number // 4), named(ordinary, number - number // 4 - 1))
    mixed = jax.random.permutation(jax.random.fold_in(own, 3), count)
    donor, taker = mixed[0:count // 2 * 2:2], mixed[1:count // 2 * 2:2]
    slack = jnp.minimum(sizes[donor] - 1, limit - sizes[taker]) // 2
    slack = jnp.where((donor == order[0]) | (taker == order[0]) | (sizes[taker] == 0), 0, jnp.maximum(slack, 0))
    shifted = jax.random.randint(jax.random.fold_in(own, 4), (count // 2,), 0, 1 << 20) % (slack + 1)
    sizes = sizes.at[donor].add(-shifted).at[taker].add(shifted)
    members = jnp.searchsorted(jnp.cumsum(sizes), jnp.arange(rows * top), side="right").astype(jnp.int32)
    table = members.reshape(top, rows).T
    table = table[jax.random.permutation(jax.random.fold_in(own, 1), rows)]
    rotation = jax.random.randint(jax.random.fold_in(own, 2), (rows, 1), 0, top)
    return jnp.take_along_axis(table, (jnp.arange(top)[None, :] + rotation) % top, axis=1)


def shares(count, total, reach, skew, full):
    portions = [(1 << 20) // math.isqrt(rank ** skew) + 1 for rank in range(1, count + 1)]
    largest = reach if full else min(reach, max(-(-total // count), total * portions[0] // sum(portions)))
    least = 1 if total - largest >= count - 1 else 0
    holding, spare = [largest] + [least] * (count - 1), total - largest - least * (count - 1)
    while spare > 0:
        free = [i for i in range(1, count) if holding[i] < largest] or [i for i in range(1, count) if holding[i] < reach]
        mass, budget = sum([portions[i] for i in free]), spare
        for i in free:
            addition = min(reach - holding[i], max(1, budget * portions[i] // mass), spare)
            holding[i] = holding[i] + addition
            spare = spare - addition
    return np.array(holding)


def scatter_about(own_key, dims, scale, reach, cuts=(), kind=jnp.bfloat16):
    result = scale * jax.random.normal(own_key, dims, jnp.float32)
    if cuts:
        result = result * block_levels(own_key, dims, cuts, -0.22, 0.18)
    return jnp.clip(result, -reach, reach).astype(kind)


def setup_inputs(seed: int = 0, part: int = 0) -> dict:
    seeds = jax.random.split(jax.random.key(seed), 8)
    own_keys = jax.random.split(jax.random.fold_in(seeds[7], part), 8)
    tokens = draw_tokens(jax.random.fold_in(jax.random.fold_in(seeds[7], part), 71), part)
    routes_keys = jax.random.split(jax.random.fold_in(own_keys[1], 1), TOKENS // TOK_FS)
    routes_turns = jax.random.permutation(jax.random.fold_in(own_keys[1], 3), TOKENS // TOK_FS)
    routes = jax.vmap(lambda own, number: assign_block(jax.random.fold_in(own_keys[1], 2), own, number, TOK_FS, EXPERTS, TOP, CAP, 1))(routes_keys, routes_turns).reshape((TOKENS, TOP))
    route_weights = jnp.clip(0.2 + 0.8 * jax.random.uniform(own_keys[2], (TOKENS, TOP), jnp.float32) ** block_levels(own_keys[2], (TOKENS, TOP), ((0, 4),), -0.2, 0.2), 0.2, 1.0)
    norm_gain = jnp.clip(1.0 + 0.18 * jax.random.normal(seeds[3], (D,), jnp.float32), 0.1, 1.9)
    gate_weight = scatter_about(seeds[4], (EXPERTS, D, FF), D ** -0.5, 0.125, ((1, 4), (2, 4)), jnp.float32)
    up_weight = scatter_about(seeds[5], (EXPERTS, D, FF), D ** -0.5, 0.125, ((1, 4), (2, 4)), jnp.float32)
    down_weight = scatter_about(seeds[6], (EXPERTS, D, FF), FF ** -0.5, 0.09375, ((1, 4), (2, 4)), jnp.float32)
    return {"tokens": tokens, "routes": routes, "route_weights": route_weights, "norm_gain": norm_gain, "gate_weight": gate_weight, "up_weight": up_weight, "down_weight": down_weight}


epsilon = 1e-06

def relayout(matrix):
    blocked = matrix.reshape(EXPERTS, D, N_TP, SUB, FFS)
    return jnp.transpose(blocked, (0, 3, 1, 2, 4)).reshape(EXPERTS * SUB, D, N_TP * FFS)

def slot_table(routes):
    blocks = routes.reshape(N_FS, TOK_FS * TOP)
    onehot = (blocks[:, :, None] == jnp.arange(EXPERTS, dtype=jnp.int32)[None, None, :]).astype(jnp.int32)
    earlier = jnp.cumsum(onehot, axis=1) - onehot
    position = lax.optimization_barrier(jnp.sum(earlier * onehot, axis=2))
    block_index = jnp.arange(N_FS, dtype=jnp.int32)[:, None]
    return (block_index * CAP + position).astype(jnp.int32).reshape(TOKENS, TOP)

def reference(tokens, routes, route_weights, norm_gain, gate_weight, up_weight, down_weight):
    gain_row = norm_gain[None, :, None]
    gate_fold = (gain_row * gate_weight).astype(jnp.bfloat16)
    up_fold = (gain_row * up_weight).astype(jnp.bfloat16)
    down_cast = down_weight.astype(jnp.bfloat16)
    widened = tokens.astype(jnp.float32)
    row_scale = lax.rsqrt(lax.optimization_barrier(jnp.mean(widened * widened, axis=1, keepdims=True)) + epsilon)
    normed = (widened * row_scale).astype(jnp.bfloat16)
    slot_place = slot_table(routes)
    token_ids = jnp.broadcast_to(jnp.arange(TOKENS, dtype=jnp.int32)[:, None], (TOKENS, TOP))
    owner_rows = jnp.zeros((EXPERTS, N_FS * CAP), jnp.int32).at[routes, slot_place].set(token_ids)

    def one_expert(expert_args):
        gate_expert, up_expert, down_expert, owner_expert = expert_args
        token_rows = normed[owner_expert]
        gate_sums = jnp.dot(token_rows, gate_expert, preferred_element_type=jnp.float32)
        up_sums = jnp.dot(token_rows, up_expert, preferred_element_type=jnp.float32)
        hidden = (jax.nn.silu(gate_sums) * up_sums).astype(jnp.bfloat16)
        blocks = hidden.reshape(N_FS * CAP, SUB * N_TP, FFS).astype(jnp.float32)
        down_blocks = down_expert.reshape(D, SUB * N_TP, FFS).astype(jnp.float32)
        partial_value = jnp.einsum('mbf,dbf->bmd', blocks, down_blocks).astype(jnp.bfloat16)
        return lax.optimization_barrier(jnp.sum(partial_value.astype(jnp.float32), axis=0))
    results = lax.map(one_expert, (gate_fold, up_fold, down_cast, owner_rows))
    selected = results[routes, slot_place]
    mixed_rows = lax.optimization_barrier(jnp.sum(route_weights[:, :, None] * selected, axis=1)).astype(jnp.bfloat16)
    return (relayout(gate_fold), relayout(up_fold), relayout(down_cast), mixed_rows)
```

```python
import functools

import jax
import jax.numpy as jnp
from jax import lax
from jax.experimental import pallas as pl
from jax.experimental.pallas import tpu as pltpu
from jax.sharding import PartitionSpec as P

epsilon = 1e-06
MESH = pl.DeviceIdType.MESH


def expert_slots(routes, experts, capacity):
    row_count = routes.shape[0] * routes.shape[1]
    flat_routes = routes.reshape(row_count)
    onehot = (flat_routes[:, None] == jnp.arange(experts, dtype=jnp.int32)[None, :]).astype(
        jnp.int32
    )
    earlier = jnp.cumsum(onehot, axis=0) - onehot
    position = jnp.sum(earlier * onehot, axis=1)
    return (flat_routes * capacity + position).reshape(routes.shape)


def dispatch(normed, slots, experts, capacity, copies, local_count):
    col_width = normed.shape[1]
    slot_ids = jnp.arange(experts * capacity, dtype=jnp.int32)
    select = jnp.any(slot_ids[:, None, None] == slots[None, :, :], axis=2).astype(jnp.bfloat16)
    packed = jnp.dot(select, normed, preferred_element_type=jnp.float32).astype(jnp.bfloat16)
    packed = jnp.broadcast_to(
        packed.reshape(experts, 1, capacity, col_width), (experts, copies, capacity, col_width)
    )
    return packed.reshape(experts * copies // local_count, local_count, capacity, col_width)


def combine(returned, slots, route_weights, experts, copies):
    capacity, col_width = (returned.shape[2], returned.shape[3])
    summed_up = jnp.sum(
        returned.reshape(experts, copies, capacity, col_width), axis=1, dtype=jnp.float32
    )
    selected = summed_up.reshape(experts * capacity, col_width)[slots]
    return jnp.sum(route_weights[:, :, None] * selected, axis=1)


def exchange_kernel(
    dims, gains, gate_w, up_w, down_w, gate_o, up_o, down_o,
    raw, stage, load_sem, send_sem, recv_sem, pass_send, pass_recv,
):
    groups, count, local, copies, rows, width, parts = dims
    weights, landing = (gate_w, up_w, down_w), (gate_o, up_o, down_o)
    y, z = lax.axis_index("grp"), lax.axis_index("fs")
    share = rows // groups
    piece = share // parts

    barrier = pltpu.get_barrier_semaphore()

    def greet(j, _):
        @pl.when(j != z)
        def _():
            pl.semaphore_signal(barrier, inc=1, device_id={"fs": j}, device_id_type=MESH)
        return 0

    lax.fori_loop(0, count, greet, 0)
    for other in range(1, groups):
        pl.semaphore_signal(
            barrier, inc=1, device_id={"grp": lax.rem(y + other, groups)}, device_id_type=MESH
        )

    def load(m, j, first, slot):
        if copies > 1:
            expert, column = j // copies, lax.rem(j, copies) * width
            column = pl.ds(pl.multiple_of(column, 128), width)
        else:
            expert, column = j * local, slice(None)
        return pltpu.make_async_copy(
            weights[m].at[pl.ds(expert, local), pl.ds(first, share), column],
            raw.at[slot], load_sem.at[slot],
        )

    def fold(m, slot, first, put):
        def one(i, _):
            l, q = i // parts, lax.rem(i, parts)
            at = pl.multiple_of(q * piece, piece)
            scaled = raw[slot, l, pl.ds(at, piece), :]
            if m < 2:
                scaled = scaled * gains[pl.ds(pl.multiple_of(first + at, piece), piece), :1]
            put(l, at, scaled.astype(jnp.bfloat16))
            return 0

        lax.fori_loop(0, local * parts, one, 0)

    def sending(j, m, i):
        l, q = i // parts, lax.rem(i, parts)
        at = pl.multiple_of(q * piece, piece)
        base = pl.multiple_of(z * rows + y * share + at, piece)
        return pltpu.make_async_remote_copy(
            src_ref=stage.at[j, m, l, pl.ds(at, piece), :],
            dst_ref=landing[m].at[l, pl.ds(base, piece), :],
            send_sem=send_sem.at[j, m, i],
            recv_sem=recv_sem.at[z, m, i],
            device_id={"fs": j}, device_id_type=MESH,
        )

    def passing(s, m, i, other):
        l, q = i // parts, lax.rem(i, parts)
        base = pl.multiple_of(s * rows + y * share + q * piece, piece)
        spot = landing[m].at[l, pl.ds(base, piece), :]
        return pltpu.make_async_remote_copy(
            src_ref=spot, dst_ref=spot,
            send_sem=pass_send.at[s, m, i, other - 1],
            recv_sem=pass_recv.at[s, m, i, other - 1],
            device_id={"grp": lax.rem(y + other, groups)}, device_id_type=MESH,
        )

    def arriving(s, m, i, other):
        l, q = i // parts, lax.rem(i, parts)
        giver = lax.rem(y + groups - other, groups)
        base = pl.multiple_of(s * rows + giver * share + q * piece, piece)
        spot = landing[m].at[l, pl.ds(base, piece), :]
        return pltpu.make_async_remote_copy(
            src_ref=spot, dst_ref=spot,
            send_sem=pass_send.at[s, m, i, other - 1],
            recv_sem=pass_recv.at[s, m, i, other - 1],
            device_id={"grp": giver}, device_id_type=MESH,
        )

    def landed(s, m, i):
        l, q = i // parts, lax.rem(i, parts)
        base = pl.multiple_of(s * rows + y * share + q * piece, piece)
        return pltpu.make_async_remote_copy(
            src_ref=landing[m].at[l, pl.ds(base, piece), :],
            dst_ref=landing[m].at[l, pl.ds(base, piece), :],
            send_sem=send_sem.at[s, m, i],
            recv_sem=recv_sem.at[s, m, i],
            device_id={"fs": s}, device_id_type=MESH,
        )

    mine = pl.multiple_of(y * share, share)
    pieces = local * parts

    def neighbours(body):
        def step(d, _):
            for j, there in ((z + d, z + d < count), (z - d, z - d >= 0)):
                @pl.when(there)
                def _():
                    body(j)
            return 0

        lax.fori_loop(1, count, step, 0)

    def send_phase(phase):
        def to(j):
            for m in phase:
                load(m, j, mine, m % 2).start()
            for m in phase:
                load(m, j, mine, m % 2).wait()

                def put(l, at, value):
                    stage[j, m, l, pl.ds(at, piece), :] = value

                fold(m, m % 2, mine, put)
            for m in phase:
                def go(i, _):
                    sending(j, m, i).start()
                    return 0

                lax.fori_loop(0, pieces, go, 0)

        neighbours(to)

    pl.semaphore_wait(barrier, count - 1 + groups - 1)
    send_phase((0, 1))
    send_phase((2,))

    for m in range(3):
        for g in range(groups):
            load(m, z, g * share, g % 2).start()
            load(m, z, g * share, g % 2).wait()

            def put(l, at, value):
                base = pl.multiple_of(z * rows + g * share + at, piece)
                landing[m][l, pl.ds(base, piece), :] = value

            fold(m, g % 2, g * share, put)

    def pass_phase(phase):
        def take(s):
            for m in phase:
                def one(i, _):
                    landed(s, m, i).wait_recv()
                    for other in range(1, groups):
                        passing(s, m, i, other).start()
                    return 0

                lax.fori_loop(0, pieces, one, 0)

        neighbours(take)

    pass_phase((0, 1))
    pass_phase((2,))

    def finish(s):
        for m in range(3):
            def one(i, _):
                for other in range(1, groups):
                    arriving(s, m, i, other).wait_recv()
                    passing(s, m, i, other).wait_send()
                sending(s, m, i).wait_send()
                return 0

            lax.fori_loop(0, pieces, one, 0)

    neighbours(finish)


def exchange(norm_gain, gate_weight, up_weight, down_weight, groups, count, copies, local):
    experts, rows, columns = gate_weight.shape
    width = columns // copies
    share = rows // groups
    parts = max(1, share // 128)
    gains = jnp.broadcast_to(norm_gain[:, None], (rows, 128))
    shape = (local, count * rows, width)
    dims = (groups, count, local, copies, rows, width, parts)
    pieces = local * parts
    return pl.pallas_call(
        functools.partial(exchange_kernel, dims),
        out_shape=[jax.ShapeDtypeStruct(shape, jnp.bfloat16)] * 3,
        in_specs=[pl.BlockSpec(memory_space=pltpu.VMEM)]
        + [pl.BlockSpec(memory_space=pl.ANY)] * 3,
        out_specs=[pl.BlockSpec(memory_space=pltpu.VMEM)] * 3,
        scratch_shapes=[
            pltpu.VMEM((2, local, share, width), jnp.float32),
            pltpu.VMEM((count, 3, local, share, width), jnp.bfloat16),
            pltpu.SemaphoreType.DMA((2,)),
            pltpu.SemaphoreType.DMA((count, 3, pieces)),
            pltpu.SemaphoreType.DMA((count, 3, pieces)),
            pltpu.SemaphoreType.DMA((count, 3, pieces, max(1, groups - 1))),
            pltpu.SemaphoreType.DMA((count, 3, pieces, max(1, groups - 1))),
        ],
        compiler_params=pltpu.CompilerParams(
            collective_id=0, has_side_effects=True, vmem_limit_bytes=60 * 1024 * 1024
        ),
    )(gains, gate_weight, up_weight, down_weight)


def on_device(tokens, routes, route_weights, norm_gain, gate_weight, up_weight, down_weight):
    groups = lax.axis_size("grp")
    fs_count = lax.axis_size("fs")
    tp_count = lax.axis_size("tp")
    experts = gate_weight.shape[0]
    copies = max(1, fs_count // experts)
    local_count = max(1, experts // fs_count)
    capacity = tokens.shape[0] * 5 // 16

    gate_new, up_new, down_new = exchange(
        norm_gain, gate_weight, up_weight, down_weight, groups, fs_count, copies, local_count
    )
    slots = expert_slots(routes, experts, capacity)
    whole = lax.all_gather(tokens, "tp", axis=1, tiled=True)
    widened = whole.astype(jnp.float32)
    row_scale = lax.rsqrt(jnp.mean(widened * widened, axis=1, keepdims=True) + epsilon)
    normed = (widened * row_scale).astype(jnp.bfloat16)
    outgoing = dispatch(normed, slots, experts, capacity, copies, local_count)
    arrived = lax.all_to_all(outgoing, "fs", split_axis=0, concat_axis=0, tiled=True)
    gate_sums = jnp.einsum("slcd,ldf->slcf", arrived, gate_new, preferred_element_type=jnp.float32)
    up_sums = jnp.einsum("slcd,ldf->slcf", arrived, up_new, preferred_element_type=jnp.float32)
    hidden = (jax.nn.silu(gate_sums) * up_sums).astype(jnp.bfloat16)
    partial_value = jnp.einsum(
        "slcf,ldf->slcd", hidden, down_new, preferred_element_type=jnp.float32
    ).astype(jnp.bfloat16)
    by_columns = partial_value.reshape(
        partial_value.shape[:3] + (tp_count, partial_value.shape[3] // tp_count)
    )
    exchanged = lax.all_to_all(by_columns, "tp", split_axis=3, concat_axis=3, tiled=True)
    summed_up = jnp.sum(exchanged, axis=3, dtype=jnp.float32)
    handed = lax.all_to_all(
        summed_up.astype(jnp.bfloat16), "fs", split_axis=0, concat_axis=0, tiled=True
    ).astype(summed_up.dtype)
    combined = combine(handed, slots, route_weights, experts, copies)
    return (gate_new, up_new, down_new, combined.astype(jnp.bfloat16))


def solution(mesh):
    in_specs = (
        P(("grp", "fs"), "tp"),
        P(("grp", "fs"), None),
        P(("grp", "fs"), None),
        P("fs"),
        P(None, "fs", "tp"),
        P(None, "fs", "tp"),
        P(None, "fs", "tp"),
    )
    out_specs = (
        P("fs", "grp", "tp"),
        P("fs", "grp", "tp"),
        P("fs", "grp", "tp"),
        P(("grp", "fs"), "tp"),
    )
    return jax.shard_map(
        on_device, mesh=mesh, in_specs=in_specs, out_specs=out_specs, check_vma=False
    )
```

```python
import functools

import jax
import jax.numpy as jnp
from jax import lax
from jax.experimental import pallas as pl
from jax.experimental.pallas import tpu as pltpu
from jax.sharding import PartitionSpec as P

epsilon = 1e-06
MESH = pl.DeviceIdType.MESH


def expert_slots(routes, experts, capacity):
    row_count = routes.shape[0] * routes.shape[1]
    flat_routes = routes.reshape(row_count)
    onehot = (flat_routes[:, None] == jnp.arange(experts, dtype=jnp.int32)[None, :]).astype(
        jnp.int32
    )
    earlier = jnp.cumsum(onehot, axis=0) - onehot
    position = jnp.sum(earlier * onehot, axis=1)
    return (flat_routes * capacity + position).reshape(routes.shape)


def dispatch(normed, slots, experts, capacity, copies, local_count):
    col_width = normed.shape[1]
    slot_ids = jnp.arange(experts * capacity, dtype=jnp.int32)
    select = jnp.any(slot_ids[:, None, None] == slots[None, :, :], axis=2).astype(jnp.bfloat16)
    packed = jnp.dot(select, normed, preferred_element_type=jnp.float32).astype(jnp.bfloat16)
    packed = jnp.broadcast_to(
        packed.reshape(experts, 1, capacity, col_width), (experts, copies, capacity, col_width)
    )
    return packed.reshape(experts * copies // local_count, local_count, capacity, col_width)


def combine(returned, slots, route_weights, experts, copies):
    capacity, col_width = (returned.shape[2], returned.shape[3])
    summed_up = jnp.sum(
        returned.reshape(experts, copies, capacity, col_width), axis=1, dtype=jnp.float32
    )
    selected = summed_up.reshape(experts * capacity, col_width)[slots]
    return jnp.sum(route_weights[:, :, None] * selected, axis=1)


def exchange_kernel(
    dims, gains, gate_w, up_w, down_w, gate_o, up_o, down_o,
    raw, stage, load_sem, send_sem, recv_sem, pass_send, pass_recv,
):
    groups, count, local, copies, rows, width, parts = dims
    weights, landing = (gate_w, up_w, down_w), (gate_o, up_o, down_o)
    y, z = lax.axis_index("grp"), lax.axis_index("fs")
    share = rows // groups
    piece = share // parts

    barrier = pltpu.get_barrier_semaphore()

    def greet(j, _):
        @pl.when(j != z)
        def _():
            pl.semaphore_signal(barrier, inc=1, device_id={"fs": j}, device_id_type=MESH)
        return 0

    lax.fori_loop(0, count, greet, 0)
    for other in range(1, groups):
        pl.semaphore_signal(
            barrier, inc=1, device_id={"grp": lax.rem(y + other, groups)}, device_id_type=MESH
        )

    def load(m, j, first, slot):
        if copies > 1:
            expert, column = j // copies, lax.rem(j, copies) * width
            column = pl.ds(pl.multiple_of(column, 128), width)
        else:
            expert, column = j * local, slice(None)
        return pltpu.make_async_copy(
            weights[m].at[pl.ds(expert, local), pl.ds(first, share), column],
            raw.at[slot], load_sem.at[slot],
        )

    def fold(m, slot, first, put):
        def one(i, _):
            l, q = i // parts, lax.rem(i, parts)
            at = pl.multiple_of(q * piece, piece)
            scaled = raw[slot, l, pl.ds(at, piece), :]
            if m < 2:
                scaled = scaled * gains[pl.ds(pl.multiple_of(first + at, piece), piece), :1]
            put(l, at, scaled.astype(jnp.bfloat16))
            return 0

        lax.fori_loop(0, local * parts, one, 0)

    def sending(j, m, i):
        l, q = i // parts, lax.rem(i, parts)
        at = pl.multiple_of(q * piece, piece)
        base = pl.multiple_of(z * rows + y * share + at, piece)
        return pltpu.make_async_remote_copy(
            src_ref=stage.at[j, m, l, pl.ds(at, piece), :],
            dst_ref=landing[m].at[l, pl.ds(base, piece), :],
            send_sem=send_sem.at[j, m, i],
            recv_sem=recv_sem.at[z, m, i],
            device_id={"fs": j}, device_id_type=MESH,
        )

    def passing(s, m, i, other):
        l, q = i // parts, lax.rem(i, parts)
        base = pl.multiple_of(s * rows + y * share + q * piece, piece)
        spot = landing[m].at[l, pl.ds(base, piece), :]
        return pltpu.make_async_remote_copy(
            src_ref=spot, dst_ref=spot,
            send_sem=pass_send.at[s, m, i, other - 1],
            recv_sem=pass_recv.at[s, m, i, other - 1],
            device_id={"grp": lax.rem(y + other, groups)}, device_id_type=MESH,
        )

    def arriving(s, m, i, other):
        l, q = i // parts, lax.rem(i, parts)
        giver = lax.rem(y + groups - other, groups)
        base = pl.multiple_of(s * rows + giver * share + q * piece, piece)
        spot = landing[m].at[l, pl.ds(base, piece), :]
        return pltpu.make_async_remote_copy(
            src_ref=spot, dst_ref=spot,
            send_sem=pass_send.at[s, m, i, other - 1],
            recv_sem=pass_recv.at[s, m, i, other - 1],
            device_id={"grp": giver}, device_id_type=MESH,
        )

    def landed(s, m, i):
        l, q = i // parts, lax.rem(i, parts)
        base = pl.multiple_of(s * rows + y * share + q * piece, piece)
        return pltpu.make_async_remote_copy(
            src_ref=landing[m].at[l, pl.ds(base, piece), :],
            dst_ref=landing[m].at[l, pl.ds(base, piece), :],
            send_sem=send_sem.at[s, m, i],
            recv_sem=recv_sem.at[s, m, i],
            device_id={"fs": s}, device_id_type=MESH,
        )

    mine = pl.multiple_of(y * share, share)
    pieces = local * parts

    def neighbours(body):
        def step(d, _):
            for j, there in ((z + d, z + d < count), (z - d, z - d >= 0)):
                @pl.when(there)
                def _():
                    body(j)
            return 0

        lax.fori_loop(1, count, step, 0)

    def send_phase(phase):
        def to(j):
            for m in phase:
                load(m, j, mine, m % 2).start()
            for m in phase:
                load(m, j, mine, m % 2).wait()

                def put(l, at, value):
                    stage[j, m, l, pl.ds(at, piece), :] = value

                fold(m, m % 2, mine, put)
            for m in phase:
                def go(i, _):
                    sending(j, m, i).start()
                    return 0

                lax.fori_loop(0, pieces, go, 0)

        neighbours(to)

    pl.semaphore_wait(barrier, count - 1 + groups - 1)
    send_phase((0, 1))
    send_phase((2,))

    for m in range(3):
        for g in range(groups):
            load(m, z, g * share, g % 2).start()
            load(m, z, g * share, g % 2).wait()

            def put(l, at, value):
                base = pl.multiple_of(z * rows + g * share + at, piece)
                landing[m][l, pl.ds(base, piece), :] = value

            fold(m, g % 2, g * share, put)

    def pass_phase(phase):
        def take(s):
            for m in phase:
                def one(i, _):
                    landed(s, m, i).wait_recv()
                    for other in range(1, groups):
                        passing(s, m, i, other).start()
                    return 0

                lax.fori_loop(0, pieces, one, 0)

        neighbours(take)

    pass_phase((0, 1))
    pass_phase((2,))

    def finish(s):
        for m in range(3):
            def one(i, _):
                for other in range(1, groups):
                    arriving(s, m, i, other).wait_recv()
                    passing(s, m, i, other).wait_send()
                sending(s, m, i).wait_send()
                return 0

            lax.fori_loop(0, pieces, one, 0)

    neighbours(finish)


def relay_kernel(
    dims, gains, gate_w, up_w, down_w, gate_o, up_o, down_o,
    raw, stage, transit, load_sem, send_sem, recv_sem, relay_sem, pass_send, pass_recv,
):
    groups, count, local, copies, rows, width, parts = dims
    weights, landing = (gate_w, up_w, down_w), (gate_o, up_o, down_o)
    y, z = lax.axis_index("grp"), lax.axis_index("fs")
    share = rows // groups
    piece = share // parts
    pieces = local * parts
    mine = pl.multiple_of(y * share, share)

    def real(way, place):
        return place if way == 0 else count - 1 - place

    barrier = pltpu.get_barrier_semaphore()
    for j, there in ((z + 1, z + 1 < count), (z - 1, z >= 1)):
        @pl.when(there)
        def _():
            pl.semaphore_signal(barrier, inc=1, device_id={"fs": j}, device_id_type=MESH)
    for other in range(1, groups):
        pl.semaphore_signal(
            barrier, inc=1, device_id={"grp": lax.rem(y + other, groups)}, device_id_type=MESH
        )

    def load(m, j, first, slot):
        if copies > 1:
            expert, column = j // copies, lax.rem(j, copies) * width
            column = pl.ds(pl.multiple_of(column, 128), width)
        else:
            expert, column = j * local, slice(None)
        return pltpu.make_async_copy(
            weights[m].at[pl.ds(expert, local), pl.ds(first, share), column],
            raw.at[slot], load_sem.at[slot],
        )

    def cut(i):
        return i // parts, pl.multiple_of(lax.rem(i, parts) * piece, piece)

    def fold(m, slot, first, put):
        def one(i, _):
            l, at = cut(i)
            scaled = raw[slot, l, pl.ds(at, piece), :]
            if m < 2:
                scaled = scaled * gains[pl.ds(pl.multiple_of(first + at, piece), piece), :1]
            put(l, at, scaled.astype(jnp.bfloat16))
            return 0

        lax.fori_loop(0, pieces, one, 0)

    def spot(m, l, at, source, giver):
        base = pl.multiple_of(source * rows + giver * share + at, piece)
        return landing[m].at[l, pl.ds(base, piece), :]

    def hop(way, src, sem, m, i, k, s, dd, final):
        l, at = cut(i)
        if final:
            dst = spot(m, l, at, real(way, s), y)
        else:
            slot = (k - s) * (count - 2 - k) + (count - 1 - dd)
            dst = transit.at[way, slot, m, l, pl.ds(at, piece), :]
        place = (k - s) * (count - 1 - k) + (count - 1 - dd)
        return pltpu.make_async_remote_copy(
            src_ref=src, dst_ref=dst, send_sem=sem,
            recv_sem=recv_sem.at[way, place, m, i],
            device_id={"fs": real(way, k + 1)}, device_id_type=MESH,
        )

    def start_hop(way, src, sem, m, i, k, s, dd):
        @pl.when(dd == k + 1)
        def _():
            hop(way, src, sem, m, i, k, s, dd, True).start()

        @pl.when(dd > k + 1)
        def _():
            hop(way, src, sem, m, i, k, s, dd, False).start()

    def passing(s, m, i, other):
        l, at = cut(i)
        ref = spot(m, l, at, s, y)
        return pltpu.make_async_remote_copy(
            src_ref=ref, dst_ref=ref,
            send_sem=pass_send.at[s, m, i, other - 1],
            recv_sem=pass_recv.at[s, m, i, other - 1],
            device_id={"grp": lax.rem(y + other, groups)}, device_id_type=MESH,
        )

    def arriving(s, m, i, other):
        l, at = cut(i)
        giver = lax.rem(y + groups - other, groups)
        ref = spot(m, l, at, s, giver)
        return pltpu.make_async_remote_copy(
            src_ref=ref, dst_ref=ref,
            send_sem=pass_send.at[s, m, i, other - 1],
            recv_sem=pass_recv.at[s, m, i, other - 1],
            device_id={"grp": giver}, device_id_type=MESH,
        )

    def send_phase(phase):
        def step(d, _):
            for way in (0, 1):
                k = real(way, z)
                dd = count - d
                j = real(way, dd)

                @pl.when(dd > k)
                def _():
                    for m in phase:
                        load(m, j, mine, m).start()
                    for m in phase:
                        load(m, j, mine, m).wait()

                        def put(l, at, value):
                            stage[j, m, l, pl.ds(at, piece), :] = value

                        fold(m, m, mine, put)

                        def go(i, _):
                            l, at = cut(i)
                            src = stage.at[j, m, l, pl.ds(at, piece), :]
                            start_hop(way, src, send_sem.at[j, m, i], m, i, k, k, dd)
                            return 0

                        lax.fori_loop(0, pieces, go, 0)
            return 0

        lax.fori_loop(1, count, step, 0)

    def own_block():
        for m in range(3):
            for g in range(groups):
                load(m, z, g * share, g % 2).start()
                load(m, z, g * share, g % 2).wait()

                def put(l, at, value):
                    stage[z, m, l, pl.ds(at, piece), :] = value

                fold(m, g % 2, g * share, put)
                base = pl.multiple_of(z * rows + g * share, share)
                keep = pltpu.make_async_copy(
                    stage.at[z, m], landing[m].at[:, pl.ds(base, share), :], load_sem.at[g % 2]
                )
                keep.start()
                keep.wait()

    def take_phase(phase):
        most = max(k * (count - k) for k in range(count))

        def take(item, _):
            for m in phase:
                def one(i, _):
                    l, at = cut(i)
                    for way in (0, 1):
                        take_piece(way, m, item, i, l, at)
                    return 0

                lax.fori_loop(0, pieces, one, 0)
            return 0

        lax.fori_loop(0, most, take, 0)

    def take_piece(way, m, item, i, l, at):
        k = real(way, z)

        @pl.when(item < k * (count - k))
        def _():
            s = k - 1 - item // (count - k)
            dd = count - 1 - lax.rem(item, count - k)
            source = real(way, s)

            def awaited(ref):
                pltpu.make_async_remote_copy(
                    src_ref=ref, dst_ref=ref, send_sem=send_sem.at[source, m, i],
                    recv_sem=recv_sem.at[way, item, m, i],
                    device_id={"fs": source}, device_id_type=MESH,
                ).wait_recv()

            @pl.when(dd == k)
            def _():
                awaited(spot(m, l, at, source, y))
                for other in range(1, groups):
                    passing(source, m, i, other).start()

            @pl.when(dd > k)
            def _():
                slot = (k - 1 - s) * (count - 1 - k) + (count - 1 - dd)
                ref = transit.at[way, slot, m, l, pl.ds(at, piece), :]
                awaited(ref)
                start_hop(way, ref, relay_sem.at[way, slot, m, i], m, i, k, s, dd)

    def sent(ref, sem):
        pltpu.make_async_remote_copy(
            src_ref=ref, dst_ref=ref, send_sem=sem, recv_sem=recv_sem.at[0, 0, 0, 0],
            device_id={"grp": lax.rem(y + 1, groups)}, device_id_type=MESH,
        ).wait_send()

    def finish():
        def block(t, _):
            s, i = t // pieces, lax.rem(t, pieces)
            l, at = cut(i)

            @pl.when(s != z)
            def _():
                for m in range(3):
                    for other in range(1, groups):
                        arriving(s, m, i, other).wait_recv()
                        passing(s, m, i, other).wait_send()
                    sent(stage.at[s, m, l, pl.ds(at, piece), :], send_sem.at[s, m, i])
            return 0

        lax.fori_loop(0, count * pieces, block, 0)

        def passed(t, _):
            slot, i = t // pieces, lax.rem(t, pieces)
            l, at = cut(i)
            for way in (0, 1):
                @pl.when(slot < z * (count - 1 - z))
                def _():
                    for m in range(3):
                        sent(
                            transit.at[way, slot, m, l, pl.ds(at, piece), :],
                            relay_sem.at[way, slot, m, i],
                        )
            return 0

        lax.fori_loop(0, transit.shape[1] * pieces, passed, 0)

    ends = (z == 0).astype(jnp.int32) + (z == count - 1).astype(jnp.int32)
    pl.semaphore_wait(barrier, 2 - ends + groups - 1)
    send_phase((0, 1, 2))
    own_block()
    take_phase((0, 1, 2))
    finish()


def exchange(norm_gain, gate_weight, up_weight, down_weight, groups, count, copies, local):
    experts, rows, columns = gate_weight.shape
    width = columns // copies
    share = rows // groups
    parts = max(1, share // 128)
    gains = jnp.broadcast_to(norm_gain[:, None], (rows, 128))
    shape = (local, count * rows, width)
    dims = (groups, count, local, copies, rows, width, parts)
    pieces = local * parts
    relaying = 1 < count <= 8 and groups > 1
    common = [
        pltpu.VMEM((3, local, share, width), jnp.float32),
        pltpu.VMEM((count, 3, local, share, width), jnp.bfloat16),
    ]
    sem = pltpu.SemaphoreType.DMA
    passes = [sem((count, 3, pieces, max(1, groups - 1)))] * 2
    if relaying:
        slots = max(1, max(k * (count - 1 - k) for k in range(count)))
        items = max(k * (count - k) for k in range(count))
        scratch = common + [
            pltpu.VMEM((2, slots, 3, local, share, width), jnp.bfloat16),
            sem((3,)), sem((count, 3, pieces)), sem((2, items, 3, pieces)),
            sem((2, slots, 3, pieces)),
        ] + passes
    else:
        scratch = common + [sem((2,))] + [sem((count, 3, pieces))] * 2 + passes
    return pl.pallas_call(
        functools.partial(relay_kernel if relaying else exchange_kernel, dims),
        out_shape=[jax.ShapeDtypeStruct(shape, jnp.bfloat16)] * 3,
        in_specs=[pl.BlockSpec(memory_space=pltpu.VMEM)]
        + [pl.BlockSpec(memory_space=pl.ANY)] * 3,
        out_specs=[pl.BlockSpec(memory_space=pl.ANY if relaying else pltpu.VMEM)] * 3,
        scratch_shapes=scratch,
        compiler_params=pltpu.CompilerParams(
            collective_id=0, has_side_effects=True, vmem_limit_bytes=60 * 1024 * 1024
        ),
    )(gains, gate_weight, up_weight, down_weight)


def on_device(tokens, routes, route_weights, norm_gain, gate_weight, up_weight, down_weight):
    groups = lax.axis_size("grp")
    fs_count = lax.axis_size("fs")
    tp_count = lax.axis_size("tp")
    experts = gate_weight.shape[0]
    copies = max(1, fs_count // experts)
    local_count = max(1, experts // fs_count)
    capacity = tokens.shape[0] * 5 // 16

    gate_new, up_new, down_new = exchange(
        norm_gain, gate_weight, up_weight, down_weight, groups, fs_count, copies, local_count
    )
    slots = expert_slots(routes, experts, capacity)
    whole = lax.all_gather(tokens, "tp", axis=1, tiled=True)
    widened = whole.astype(jnp.float32)
    row_scale = lax.rsqrt(jnp.mean(widened * widened, axis=1, keepdims=True) + epsilon)
    normed = (widened * row_scale).astype(jnp.bfloat16)
    outgoing = dispatch(normed, slots, experts, capacity, copies, local_count)
    arrived = lax.all_to_all(outgoing, "fs", split_axis=0, concat_axis=0, tiled=True)
    gate_sums = jnp.einsum("slcd,ldf->slcf", arrived, gate_new, preferred_element_type=jnp.float32)
    up_sums = jnp.einsum("slcd,ldf->slcf", arrived, up_new, preferred_element_type=jnp.float32)
    hidden = (jax.nn.silu(gate_sums) * up_sums).astype(jnp.bfloat16)
    partial_value = jnp.einsum(
        "slcf,ldf->slcd", hidden, down_new, preferred_element_type=jnp.float32
    ).astype(jnp.bfloat16)
    by_columns = partial_value.reshape(
        partial_value.shape[:3] + (tp_count, partial_value.shape[3] // tp_count)
    )
    exchanged = lax.all_to_all(by_columns, "tp", split_axis=3, concat_axis=3, tiled=True)
    summed_up = jnp.sum(exchanged, axis=3, dtype=jnp.float32)
    handed = lax.all_to_all(
        summed_up.astype(jnp.bfloat16), "fs", split_axis=0, concat_axis=0, tiled=True
    ).astype(summed_up.dtype)
    combined = combine(handed, slots, route_weights, experts, copies)
    return (gate_new, up_new, down_new, combined.astype(jnp.bfloat16))


def solution(mesh):
    in_specs = (
        P(("grp", "fs"), "tp"),
        P(("grp", "fs"), None),
        P(("grp", "fs"), None),
        P("fs"),
        P(None, "fs", "tp"),
        P(None, "fs", "tp"),
        P(None, "fs", "tp"),
    )
    out_specs = (
        P("fs", "grp", "tp"),
        P("fs", "grp", "tp"),
        P("fs", "grp", "tp"),
        P(("grp", "fs"), "tp"),
    )
    return jax.shard_map(
        on_device, mesh=mesh, in_specs=in_specs, out_specs=out_specs, check_vma=False
    )
```
